32 devices in a mesh: grp: 2 (over x), ep: 8 (over z, y), tp: 2 (over core).
Axes of the slice: x: 2, y: 2, z: 4, core: 2. Of those that a mesh axis runs over, the one named last changes fastest.
Arguments:
- tokens: bfloat16 [512, 2048], P(('grp', 'ep'), 'tp'), parts along dimension 0, may hold values from -6 to 6
- routes: int32 [512, 4], P(('grp', 'ep')), parts along dimension 0, may hold values from 0 to 7, all different within a row; in each aligned block of 32 rows (0 to 31, 32 to 63, ...) at most 18 rows name the same one
- gate_logits: float32 [512, 4], P(('grp', 'ep')), parts along dimension 0, may hold values from -6 to 6
- norm_gain: float32 [2048], P('tp'), may hold values from 0.1 to 1.9
- norm_shift: float32 [2048], P('tp'), may hold values from -3 to 3
- gate_weight: bfloat16 [8, 2048, 1024], P('ep', None, 'tp'), may hold values from -0.5 to 0.5
- up_weight: bfloat16 [8, 2048, 1024], P('ep', None, 'tp'), may hold values from -0.5 to 0.5
- down_weight: bfloat16 [8, 1024, 2048], P('ep', 'tp'), may hold values from -0.0234375 to 0.0234375
Outputs:
- mixed: bfloat16 [512, 2048], P(('grp', 'ep'), 'tp'), parts along dimension 0
The draws below stay inside these ranges and needn't reach their ends.
There are 2 independent parts, one for each index of `grp`. The reference program is written for one: setup_inputs(seed, part) draws one part's arguments, and reference() takes and returns one part's arrays. A program takes and returns all parts, laid end to end along the dimension named above; an argument that names none is the same for every part. Nothing has to cross between parts.
Inputs may be any that keep to these rules, and one draw needn't show every extreme that they name: `routes`: each row names 4 different experts. Within the 32 rows of one index of ep no expert is named more than 18 times, a bound that some blocks reach.
All inputs are finite; a program needn't handle non-finite values.
Results may differ from the reference program's by a relative error of at most 0.012.
Values may be sent and summed in bfloat16 or wider, within the bound.
A program may use at most 64 MiB of HBM per device.

```python
import math
import jax
import jax.numpy as jnp
import numpy as np
from jax import lax

D = 2048
FF = 1024
TOP_K = 4
TOK_DEV = 32
EXPERTS = 8
CAP = 18
SLOTS = 144
TOKENS = 256
N_EP = 8
N_TP = 2


def shard_levels(own_key, dims, pieces, least, top_value):
    factor_of, own = 1.0, jax.random.fold_in(own_key, 6)
    for position, blocks in pieces:
        heights = jnp.exp(jax.random.uniform(jax.random.fold_in(own, position), (blocks,), jnp.float32, least / len(pieces), top_value / len(pieces)))
        factor_of = factor_of * jnp.repeat(heights, dims[position] // blocks).reshape([-1 if axis == position else 1 for axis in range(len(dims))])
    return factor_of


def shared_out(stream_key, own, number, rows, amount, top, limit, lean):
    ranking = jax.random.permutation(stream_key, amount)
    crowded, common = shares(amount, rows * top, limit, lean, True), shares(amount, rows * top, limit, lean, False)
    places = jnp.arange(amount)

    def named(sizes, rotation):
        used = int((sizes > 0).sum())
        fixed = max(1, used // 4)
        passed = fixed + (places - fixed + rotation * (used - fixed)) % max(1, amount - fixed)
        return jnp.zeros((amount,), jnp.int32).at[ranking[jnp.where(places < fixed, places, passed)]].set(jnp.asarray(sizes, jnp.int32))

    sizes = jnp.where(number % 4 == 0, named(crowded, number // 4), named(common, number - number // 4 - 1))
    mixed = jax.random.permutation(jax.random.fold_in(own, 3), amount)
    giver, sink = mixed[0:amount // 2 * 2:2], mixed[1:amount // 2 * 2:2]
    margin = jnp.minimum(sizes[giver] - 1, limit - sizes[sink]) // 2
    margin = jnp.where((giver == ranking[0]) | (sink == ranking[0]) | (sizes[sink] == 0), 0, jnp.maximum(margin, 0))
    passed = jax.random.randint(jax.random.fold_in(own, 4), (amount // 2,), 0, 1 << 20) % (margin + 1)
    sizes = sizes.at[giver].add(-passed).at[sink].add(passed)
    labels = jnp.searchsorted(jnp.cumsum(sizes), jnp.arange(rows * top), side="right").astype(jnp.int32)
    table = labels.reshape(top, rows).T
    table = table[jax.random.permutation(jax.random.fold_in(own, 1), rows)]
    rotation = jax.random.randint(jax.random.fold_in(own, 2), (rows, 1), 0, top)
    return jnp.take_along_axis(table, (jnp.arange(top)[None, :] + rotation) % top, axis=1)


def shares(amount, total, reach, slope, full):
    portions = [(1 << 20) // math.isqrt(grade ** slope) + 1 for grade in range(1, amount + 1)]
    largest = reach if full else min(reach, max(-(-total // amount), total * portions[0] // sum(portions)))
    least = 1 if total - largest >= amount - 1 else 0
    given, spare = [largest] + [least] * (amount - 1), total - largest - least * (amount - 1)
    while spare > 0:
        candidates = [i for i in range(1, amount) if given[i] < largest] or [i for i in range(1, amount) if given[i] < reach]
        whole, remaining = sum([portions[i] for i in candidates]), spare
        for i in candidates:
            more = min(reach - given[i], max(1, remaining * portions[i] // whole), spare)
            given[i] = given[i] + more
            spare = spare - more
    return np.array(given)


def gaussian(own_key, extent, scale, most, cuts=(), kind=jnp.bfloat16):
    entries = scale * jax.random.normal(own_key, extent, jnp.float32)
    if cuts:
        entries = entries * shard_levels(own_key, extent, cuts, -0.22, 0.18)
    return jnp.clip(entries, -most, most).astype(kind)


def setup_inputs(seed: int = 0, part: int = 0) -> dict:
    key_list = jax.random.split(jax.random.key(seed), 9)
    part_splits = jax.random.split(jax.random.fold_in(key_list[8], part), 9)
    tokens = gaussian(part_splits[0], (TOKENS, D), 1.0, 6.0, ((0, 8), (1, 2)))
    routes_keys = jax.random.split(jax.random.fold_in(part_splits[1], 1), TOKENS // TOK_DEV)
    routes_turns = jax.random.permutation(jax.random.fold_in(part_splits[1], 3), TOKENS // TOK_DEV)
    routes = jax.vmap(lambda own, number: shared_out(jax.random.fold_in(part_splits[1], 2), own, number, TOK_DEV, EXPERTS, TOP_K, CAP, 2))(routes_keys, routes_turns).reshape((TOKENS, TOP_K))
    gate_logits = gaussian(part_splits[2], (TOKENS, TOP_K), 1.5, 6.0, ((0, 8),), jnp.float32)
    norm_gain = jnp.clip(1.0 + 0.18 * jax.random.normal(key_list[3], (D,), jnp.float32), 0.1, 1.9)
    norm_shift = gaussian(key_list[4], (D,), 0.5, 3.0, ((0, 2),), jnp.float32)
    gate_weight = gaussian(key_list[5], (EXPERTS, D, FF), (D // 16) ** -0.5, 0.5, ((0, 8), (2, 2)))
    up_weight = gaussian(key_list[6], (EXPERTS, D, FF), (D // 16) ** -0.5, 0.5, ((0, 8), (2, 2)))
    down_weight = gaussian(key_list[7], (EXPERTS, FF, D), (FF * 64) ** -0.5, 0.0234375, ((0, 8), (1, 2)))
    return {"tokens": tokens, "routes": routes, "gate_logits": gate_logits, "norm_gain": norm_gain, "norm_shift": norm_shift, "gate_weight": gate_weight, "up_weight": up_weight, "down_weight": down_weight}


norm_eps = 1e-05
clamp_limit = 7.0
sigmoid_slope = 1.702

def one_expert(operands):
    row_block, gate_mat, up_mat, down_mat = operands
    gate_pre = jnp.dot(row_block, gate_mat, preferred_element_type=jnp.float32)
    up_pre = jnp.dot(row_block, up_mat, preferred_element_type=jnp.float32)
    gate_cut = jnp.minimum(gate_pre, clamp_limit)
    up_cut = jnp.clip(up_pre, -clamp_limit, clamp_limit)
    hidden = ((up_cut + 1.0) * gate_cut * jax.nn.sigmoid(sigmoid_slope * gate_cut)).astype(jnp.bfloat16)
    portion_width = FF // N_TP
    running = jnp.zeros((row_block.shape[0], D), jnp.float32)
    for portion in range(N_TP):
        lower = portion * portion_width
        partial_out = jnp.dot(hidden[:, lower:lower + portion_width], down_mat[lower:lower + portion_width], preferred_element_type=jnp.float32).astype(jnp.bfloat16)
        partial_out = lax.optimization_barrier(partial_out)
        running = running + partial_out.astype(jnp.float32)
    return running.astype(jnp.bfloat16)

def reference(tokens, routes, gate_logits, norm_gain, norm_shift, gate_weight, up_weight, down_weight):
    floats = tokens.astype(jnp.float32)
    average = lax.optimization_barrier(jnp.sum(floats, axis=1)) / D
    variance = lax.optimization_barrier(jnp.sum(floats * floats, axis=1)) / D - average * average
    normed = ((floats - average[:, None]) * lax.rsqrt(variance[:, None] + norm_eps) * norm_gain + norm_shift).astype(jnp.bfloat16)
    exp_logits = jnp.exp(gate_logits)
    weights = exp_logits / lax.optimization_barrier(jnp.sum(exp_logits, axis=1, keepdims=True))
    flat_experts = routes.reshape(N_EP, TOK_DEV * TOP_K)
    onehot = (flat_experts[:, :, None] == jnp.arange(EXPERTS, dtype=jnp.int32)[None, None, :]).astype(jnp.int32)
    rank_in = lax.optimization_barrier(jnp.sum((jnp.cumsum(onehot, axis=1) - onehot) * onehot, axis=2))
    source = jnp.arange(N_EP, dtype=jnp.int32)[:, None]
    slot_index = (flat_experts * SLOTS + source * CAP + rank_in).reshape(TOKENS * TOP_K).astype(jnp.int32)
    token_index = jnp.arange(TOKENS * TOP_K, dtype=jnp.int32) // TOP_K
    slot_token = jnp.full((EXPERTS * SLOTS,), TOKENS, jnp.int32).at[slot_index].set(token_index)
    padded = jnp.concatenate([normed, jnp.zeros((1, D), jnp.bfloat16)], axis=0)
    row_blocks = padded[slot_token].reshape(EXPERTS, SLOTS, D)
    expert_out = lax.map(one_expert, (row_blocks, gate_weight, up_weight, down_weight)).reshape(EXPERTS * SLOTS, D)
    picked = expert_out[slot_index].astype(jnp.float32).reshape(TOKENS, TOP_K, D)
    return lax.optimization_barrier(jnp.sum(picked * weights[:, :, None], axis=1)).astype(jnp.bfloat16)
```

```python
import functools

import jax
import jax.numpy as jnp
from jax import lax
from jax.experimental import pallas as pl
from jax.experimental.pallas import tpu as pltpu
from jax.sharding import PartitionSpec as P

norm_eps = 1e-05
clamp_limit = 7.0
sigmoid_slope = 1.702
MESH = pl.DeviceIdType.MESH
f32 = jnp.float32
bf16 = jnp.bfloat16


def kernel(
    n, cap, pad,
    tokens_ref, routes_ref, logits_ref, gain_ref, shift_ref, wg_hbm, wu_hbm, wd_hbm,
    out_ref,
    wg, wu, wd, stat_out, stat_in, outb, rows, part_out, part_in, answer, back,
    w_sem, st_sem, d_send, d_recv, f_send, f_recv, p_send, p_recv, r_send, r_recv,
):
    me = lax.axis_index("ep")
    tp = lax.axis_index("tp")
    other = 1 - tp
    half = tokens_ref.shape[1]
    width = 2 * half
    toks, top = routes_ref.shape
    slots = n * pad
    paired = n & (n - 1) == 0

    def peer(d, sign):
        if not paired:
            return lax.rem(me + sign * d + n, n)
        where, bit = me, 1
        while bit < n:
            if d & bit:
                where = where + bit * (1 - 2 * lax.rem(me // bit, 2))
            bit *= 2
        return where

    order = list(range(n - 1, 0, -1))
    target = [me] + [peer(d, 1) for d in range(1, n)]
    source = [me] + [peer(d, -1) for d in range(1, n)]

    barrier = pltpu.get_barrier_semaphore()
    pl.semaphore_signal(barrier, inc=1, device_id={"tp": other}, device_id_type=MESH)
    for d in order:
        pl.semaphore_signal(barrier, inc=1, device_id={"ep": target[d]}, device_id_type=MESH)
    loads = [
        pltpu.make_async_copy(wg_hbm.at[0], wg, w_sem.at[0]),
        pltpu.make_async_copy(wu_hbm.at[0], wu, w_sem.at[1]),
        pltpu.make_async_copy(wd_hbm.at[0], wd, w_sem.at[2]),
    ]
    for load in loads:
        load.start()

    x = tokens_ref[...].astype(f32)
    sum_one = jnp.sum(x, axis=1, keepdims=True)
    sum_two = jnp.sum(x * x, axis=1, keepdims=True)
    lane = lax.broadcasted_iota(jnp.int32, (toks, 128), 1)
    stat_out[...] = jnp.where(lane == 0, sum_one, sum_two)

    column = lax.broadcasted_iota(jnp.int32, (toks, slots), 1)
    expert, rank = column // pad, column % pad
    logits = jnp.exp(logits_ref[...])
    weights = logits / jnp.sum(logits, axis=1, keepdims=True)
    routes = routes_ref[...]
    named = jnp.zeros((toks, slots), f32)
    share = jnp.zeros((toks, slots), f32)
    for k in range(top):
        hit = routes[:, k:k + 1] == expert
        named = jnp.where(hit, 1.0, named)
        share = jnp.where(hit, weights[:, k:k + 1], share)
    earlier = (
        lax.broadcasted_iota(jnp.int32, (toks, toks), 1)
        < lax.broadcasted_iota(jnp.int32, (toks, toks), 0)
    )
    ranks = jnp.dot(
        jnp.where(earlier, 1.0, 0.0).astype(bf16), named.astype(bf16), preferred_element_type=f32
    )
    chosen = (named > 0.5) & (ranks == rank.astype(f32))
    share = jnp.where(chosen, share, 0.0)
    pick = jnp.transpose(jnp.where(chosen, 1.0, 0.0)).astype(bf16)
    share_a = share.astype(bf16)
    rest = share - share_a.astype(f32)
    share_b = rest.astype(bf16)
    share_c = (rest - share_b.astype(f32)).astype(bf16)

    back[...] = jnp.zeros_like(back)
    pl.semaphore_wait(barrier, n)

    stat = pltpu.make_async_remote_copy(
        stat_out, stat_in, st_sem.at[0], st_sem.at[1], device_id={"tp": other}, device_id_type=MESH
    )
    stat.start()
    stat.wait()
    average = (sum_one + stat_in[:, 0:1]) / width
    variance = (sum_two + stat_in[:, 1:2]) / width - average * average
    normed = (
        (x - average) * lax.rsqrt(variance + norm_eps) * gain_ref[...] + shift_ref[...]
    ).astype(bf16)
    outb[...] = jnp.dot(pick, normed, preferred_element_type=f32).astype(bf16).reshape(n, pad, half)

    def dispatch(d):
        return pltpu.make_async_remote_copy(
            outb.at[target[d], pl.ds(0, cap)], rows.at[tp, me, pl.ds(0, cap)],
            d_send.at[d], d_recv.at[d], device_id={"ep": target[d]}, device_id_type=MESH,
        )

    def forward(d):
        spot = rows.at[tp, source[d], pl.ds(0, cap)]
        return pltpu.make_async_remote_copy(
            spot, spot, f_send.at[d], f_recv.at[d], device_id={"tp": other}, device_id_type=MESH
        )

    for d in order:
        dispatch(d).start()
    rows[tp, me] = outb[me]
    forward(0).start()
    for d in reversed(order):
        dispatch(d).wait_recv()
        forward(d).start()
    for load in loads:
        load.wait()
    for d in range(n):
        forward(d).wait_recv()

    ff = wg.shape[1]
    left = rows[0].reshape(slots, half)
    right = rows[1].reshape(slots, half)
    gate = jnp.dot(left, wg[:half], preferred_element_type=f32) + jnp.dot(
        right, wg[half:], preferred_element_type=f32
    )
    up = jnp.dot(left, wu[:half], preferred_element_type=f32) + jnp.dot(
        right, wu[half:], preferred_element_type=f32
    )
    cut = jnp.minimum(gate, clamp_limit)
    hidden = (
        (jnp.clip(up, -clamp_limit, clamp_limit) + 1.0) * cut * jax.nn.sigmoid(sigmoid_slope * cut)
    ).astype(bf16)

    def columns(index):
        return pl.ds(pl.multiple_of(index * half, half), half)

    part_out[...] = (
        jnp.dot(hidden, wd[:, columns(other)], preferred_element_type=f32)
        .astype(bf16).reshape(n, pad, half)
    )

    def partial(d):
        return pltpu.make_async_remote_copy(
            part_out.at[source[d], pl.ds(0, cap)], part_in.at[source[d], pl.ds(0, cap)],
            p_send.at[d], p_recv.at[d], device_id={"tp": other}, device_id_type=MESH,
        )

    def give_back(d):
        return pltpu.make_async_remote_copy(
            answer.at[source[d], pl.ds(0, cap)], back.at[me, pl.ds(0, cap)],
            r_send.at[d], r_recv.at[d], device_id={"ep": source[d]}, device_id_type=MESH,
        )

    for d in order + [0]:
        partial(d).start()
    answer[...] = (
        jnp.dot(hidden, wd[:, columns(tp)], preferred_element_type=f32)
        .astype(bf16).reshape(n, pad, half)
    )
    for d in order + [0]:
        partial(d).wait_recv()
        spot = source[d]
        total = (
            answer[spot, pl.ds(0, cap)].astype(f32) + part_in[spot, pl.ds(0, cap)].astype(f32)
        ).astype(bf16)
        if d:
            answer[spot, pl.ds(0, cap)] = total
            give_back(d).start()
        else:
            back[me, pl.ds(0, cap)] = total
    for d in reversed(order):
        give_back(d).wait_recv()
    got = back[...].reshape(slots, half)
    mixed = (
        jnp.dot(share_c, got, preferred_element_type=f32)
        + jnp.dot(share_b, got, preferred_element_type=f32)
        + jnp.dot(share_a, got, preferred_element_type=f32)
    )
    out_ref[...] = mixed.astype(bf16)
    for d in range(n):
        forward(d).wait_send()
        partial(d).wait_send()
        if d:
            dispatch(d).wait_send()
            give_back(d).wait_send()


def body(tokens, routes, gate_logits, norm_gain, norm_shift, gate_weight, up_weight, down_weight):
    n = lax.axis_size("ep")
    toks, top = routes.shape
    half = tokens.shape[1]
    cap = toks * top // n + 2
    pad = -(-cap // 16) * 16
    cap = -(-cap // 8) * 8
    ff = gate_weight.shape[2]
    vmem = pl.BlockSpec(memory_space=pltpu.VMEM)
    hbm = pl.BlockSpec(memory_space=pl.ANY)
    block = pltpu.VMEM((n, pad, half), bf16)
    sems = pltpu.SemaphoreType.DMA((n,))
    return pl.pallas_call(
        functools.partial(kernel, n, cap, pad),
        out_shape=jax.ShapeDtypeStruct((toks, half), bf16),
        in_specs=[vmem] * 5 + [hbm] * 3,
        out_specs=vmem,
        scratch_shapes=[
            pltpu.VMEM((2 * half, ff), bf16),
            pltpu.VMEM((2 * half, ff), bf16),
            pltpu.VMEM((ff, 2 * half), bf16),
            pltpu.VMEM((toks, 128), f32),
            pltpu.VMEM((toks, 128), f32),
            block,
            pltpu.VMEM((2, n, pad, half), bf16),
            block, block, block, block,
            pltpu.SemaphoreType.DMA((3,)),
            pltpu.SemaphoreType.DMA((2,)),
            sems, sems, sems, sems, sems, sems, sems, sems,
        ],
        compiler_params=pltpu.CompilerParams(collective_id=0, has_side_effects=True),
    )(
        tokens, routes, gate_logits, norm_gain.reshape(1, half), norm_shift.reshape(1, half),
        gate_weight, up_weight, down_weight,
    )


def solution(mesh):
    placed = (
        P(("grp", "ep"), "tp"),
        P(("grp", "ep"), None),
        P(("grp", "ep"), None),
        P("tp"),
        P("tp"),
        P("ep", None, "tp"),
        P("ep", None, "tp"),
        P("ep", "tp", None),
    )
    return jax.shard_map(
        body, mesh=mesh, in_specs=placed, out_specs=P(("grp", "ep"), "tp"), check_vma=False
    )
```

```python
import functools

import jax
import jax.numpy as jnp
from jax import lax
from jax.experimental import pallas as pl
from jax.experimental.pallas import tpu as pltpu
from jax.sharding import PartitionSpec as P

norm_eps = 1e-05
clamp_limit = 7.0
sigmoid_slope = 1.702
MESH = pl.DeviceIdType.MESH
LANES = 128
f32 = jnp.float32
bf16 = jnp.bfloat16


def dot(a, b):
    return jnp.dot(a, b, preferred_element_type=f32)


def iota(shape, axis):
    return lax.broadcasted_iota(jnp.int32, shape, axis)


def kernel(
    n, base, rem, seq, groups, sends,
    tokens_hbm, routes_hbm, logits_hbm, gain_hbm, shift_hbm, wg_hbm, wu_hbm, wd_hbm,
    out_ref,
    tok, routes_ref, logits_ref, affine, wg, wu, wd,
    outb1, outb2, rows1, rows2, part_out, part_in, ans1, ans2, back1, back2,
    i_sem, w_sem, a_sem, d_send, d_recv, f_send, f_recv, p_send, p_recv, r_send, r_recv,
):
    me = lax.axis_index("ep")
    tp = lax.axis_index("tp")
    other = 1 - tp
    toks, half = tok.shape
    width = 2 * half
    top = routes_ref.shape[0]
    chunks = half // LANES
    spread = rem * chunks
    paired = n & (n - 1) == 0
    parts = 2 if rem else 1

    def peer(d, sign):
        if not paired:
            return lax.rem(me + sign * d + n, n)
        where, bit = me, 1
        while bit < n:
            if d & bit:
                where = where + bit * (1 - 2 * lax.rem(me // bit, 2))
            bit *= 2
        return where

    target = [peer(d, 1) for d in seq]
    source = [peer(d, -1) for d in seq]

    barrier = pltpu.get_barrier_semaphore()
    for i in sends:
        pl.semaphore_signal(barrier, inc=1, device_id={"ep": target[i]}, device_id_type=MESH)
    pl.semaphore_signal(barrier, inc=1, device_id={"tp": other}, device_id_type=MESH)

    first = [
        pltpu.make_async_copy(routes_hbm, routes_ref, i_sem.at[0]),
        pltpu.make_async_copy(tokens_hbm, tok, i_sem.at[1]),
        pltpu.make_async_copy(logits_hbm, logits_ref, i_sem.at[2]),
        pltpu.make_async_copy(gain_hbm, affine.at[0, 0], i_sem.at[3]),
        pltpu.make_async_copy(shift_hbm, affine.at[0, 1], i_sem.at[4]),
    ]
    loads = []
    for j, side in enumerate((tp, other)):
        span = pl.ds(pl.multiple_of(side * half, half), half)
        loads += [
            pltpu.make_async_copy(wg_hbm.at[0, span], wg.at[j], w_sem.at[3 * j]),
            pltpu.make_async_copy(wu_hbm.at[0, span], wu.at[j], w_sem.at[3 * j + 1]),
            pltpu.make_async_copy(wd_hbm.at[0, :, span], wd.at[j], w_sem.at[3 * j + 2]),
        ]
    for load in first + loads:
        load.start()
    for load in first:
        load.wait()

    routes = routes_ref[...]
    logits = jnp.exp(logits_ref[...])
    weights = logits / jnp.sum(logits, axis=0, keepdims=True)
    before = jnp.where(iota((toks, toks), 0) < iota((toks, toks), 1), 1.0, 0.0).astype(bf16)

    def choose(place, rank):
        shape = place.shape
        expert = jnp.zeros(shape, jnp.int32)
        for i in range(n):
            expert = jnp.where(place == i, target[i], expert)
        named = jnp.zeros(shape, f32)
        share = jnp.zeros(shape, f32)
        for k in range(top):
            hit = routes[k:k + 1, :] == expert
            named = jnp.where(hit, 1.0, named)
            share = jnp.where(hit, weights[k:k + 1, :], share)
        chosen = (named > 0.5) & (dot(named.astype(bf16), before) == rank.astype(f32))
        return jnp.where(chosen, 1.0, 0.0), jnp.where(chosen, share, 0.0)

    def split(share):
        whole = jnp.transpose(share)
        a = whole.astype(bf16)
        rest = whole - a.astype(f32)
        b = rest.astype(bf16)
        return a, b, (rest - b.astype(f32)).astype(bf16)

    row = iota((n * base, toks), 0)
    pick, share = choose(row // base, row % base)
    outb1[...] = dot(pick.astype(bf16), tok[...]).astype(bf16).reshape(n, base, half)
    share_main = split(share)
    if rem:
        row = iota((n * spread, toks), 0)
        pick, _ = choose(row // spread, base + row % rem)
        chunk = row % spread // rem
        total = jnp.zeros((n * spread, LANES), f32)
        for c in range(chunks):
            total += dot(
                jnp.where(chunk == c, pick, 0.0).astype(bf16), tok[:, c * LANES:(c + 1) * LANES]
            )
        outb2[...] = total.astype(bf16).reshape(n, spread, LANES)
        row = iota((n * rem, toks), 0)
        _, share = choose(row // rem, base + row % rem)
        share_extra = split(share)

    def unpack(flat, count):
        size = count * spread
        r, z = iota((size, size), 0), iota((size, size), 1)
        c, q = r // (count * rem), r % (count * rem)
        where = q // rem * spread + c * rem + q % rem
        rows = dot(jnp.where(where == z, 1.0, 0.0).astype(bf16), flat)
        block = count * rem
        return jnp.concatenate([rows[c * block:(c + 1) * block] for c in range(chunks)], axis=1)

    def repack(rows, count):
        size = count * spread
        z, r = iota((size, size), 0), iota((size, size), 1)
        c, q = r // (count * rem), r % (count * rem)
        where = q // rem * spread + c * rem + q % rem
        flat = jnp.concatenate(
            [rows[:, c * LANES:(c + 1) * LANES] for c in range(chunks)], axis=0
        ).astype(bf16)
        return dot(jnp.where(where == z, 1.0, 0.0).astype(bf16), flat).astype(bf16)

    def across(src, dst, i, part, send, recv, place):
        return pltpu.make_async_remote_copy(
            src, dst, send.at[2 * i + part], recv.at[2 * i + part], device_id=place,
            device_id_type=MESH,
        )

    def dispatch(i):
        place = {"ep": target[i]}
        pieces = [(outb1, rows1), (outb2, rows2)][:parts]
        return [
            across(a.at[i], b.at[0, i], i, p, d_send, d_recv, place)
            for p, (a, b) in enumerate(pieces)
        ]

    def forward(i):
        place = {"tp": other}
        pieces = [(outb1, rows1), (outb2, rows2)][:parts]
        return [
            across(b.at[0, i] if i else a.at[i], b.at[1, i], i, p, f_send, f_recv, place)
            for p, (a, b) in enumerate(pieces)
        ]

    def give_back(i):
        place = {"ep": source[i]}
        pieces = [(ans1, back1), (ans2, back2)][:parts]
        return [
            across(a.at[i], b.at[i], i, p, r_send, r_recv, place)
            for p, (a, b) in enumerate(pieces)
        ]

    def partial(g):
        return pltpu.make_async_remote_copy(
            part_out.at[g], part_in.at[g], p_send.at[g], p_recv.at[g], device_id={"tp": other},
            device_id_type=MESH,
        )

    affine_copy = pltpu.make_async_remote_copy(
        affine.at[0], affine.at[1], a_sem.at[0], a_sem.at[1], device_id={"tp": other},
        device_id_type=MESH,
    )

    pl.semaphore_wait(barrier, n)
    for i in sends:
        for copy in dispatch(i):
            copy.start()
    for copy in forward(0):
        copy.start()
    affine_copy.start()
    rows1[0, 0] = outb1[0]
    if rem:
        rows2[0, 0] = outb2[0]
    for load in loads:
        load.wait()
    affine_copy.wait_recv()

    def landed(g):
        lower, upper = groups[g]
        for i in [i for i in [0] + sends if lower <= i < upper and i]:
            for arrived, onward in zip(dispatch(i), forward(i)):
                arrived.wait_recv()
                onward.start()

    def gathered(j, lower, upper):
        count = upper - lower
        main = rows1[j, lower:upper].reshape(count * base, half).astype(f32)
        if not rem:
            return main
        extra = unpack(rows2[j, lower:upper].reshape(count * spread, LANES), count)
        return jnp.concatenate([main, extra], axis=0)

    def experts(g):
        lower, upper = groups[g]
        for i in range(lower, upper):
            for copy in forward(i):
                copy.wait_recv()
        x = [gathered(j, lower, upper) for j in range(2)]
        average = (
            jnp.sum(x[0], axis=1, keepdims=True) + jnp.sum(x[1], axis=1, keepdims=True)
        ) / width
        squares = (
            jnp.sum(x[0] * x[0], axis=1, keepdims=True)
            + jnp.sum(x[1] * x[1], axis=1, keepdims=True)
        ) / width
        scale = lax.rsqrt(squares - average * average + norm_eps)
        normed = [
            ((x[j] - average) * scale * affine[j, 0] + affine[j, 1]).astype(bf16)
            for j in range(2)
        ]
        gate = dot(normed[0], wg[0]) + dot(normed[1], wg[1])
        up = dot(normed[0], wu[0]) + dot(normed[1], wu[1])
        cut = jnp.minimum(gate, clamp_limit)
        hidden = (
            (jnp.clip(up, -clamp_limit, clamp_limit) + 1.0)
            * cut * jax.nn.sigmoid(sigmoid_slope * cut)
        ).astype(bf16)
        part_out[g] = dot(hidden, wd[1]).astype(bf16)
        partial(g).start()
        return dot(hidden, wd[0]).astype(bf16)

    def answer(g, mine):
        lower, upper = groups[g]
        count = upper - lower
        partial(g).wait_recv()
        total = (mine.astype(f32) + part_in[g].astype(f32)).astype(bf16)
        ans1[lower:upper] = total[:count * base].reshape(count, base, half)
        if rem:
            ans2[lower:upper] = repack(total[count * base:].astype(f32), count).reshape(
                count, spread, LANES
            )
        if lower == 0:
            back1[0] = ans1[0]
            if rem:
                back2[0] = ans2[0]
        for i in sends:
            if lower <= i < upper:
                for copy in give_back(i):
                    copy.start()

    for g in range(len(groups)):
        landed(g)
        answer(g, experts(g))
    for i in sends:
        for copy in give_back(i):
            copy.wait_recv()
    got = back1[...].reshape(n * base, half)
    mixed = dot(share_main[2], got) + dot(share_main[1], got) + dot(share_main[0], got)
    if rem:
        got = unpack(back2[...].reshape(n * spread, LANES), n).astype(bf16)
        mixed += dot(share_extra[2], got) + dot(share_extra[1], got) + dot(share_extra[0], got)
    out_ref[...] = mixed.astype(bf16)
    affine_copy.wait_send()
    for g in range(len(groups)):
        partial(g).wait_send()
    for i in range(n):
        for copy in forward(i) + (dispatch(i) + give_back(i) if i else []):
            copy.wait_send()


def body(tokens, routes, gate_logits, norm_gain, norm_shift, gate_weight, up_weight, down_weight):
    n = lax.axis_size("ep")
    toks, top = routes.shape
    half = tokens.shape[1]
    cap = toks * top // n + 2
    base, rem = cap // 8 * 8, cap % 8
    if base == 0 or rem > 4:
        base, rem = -(-cap // 8) * 8, 0
    ff = gate_weight.shape[2]
    if n % 4 == 0:
        q = n // 4
        seq = [*range(q), *range(2 * q, 3 * q), *range(3 * q, n), *range(q, 2 * q)]
        groups = [(0, 2 * q), (2 * q, n)]
        sends = [*range(q, 2 * q), *range(1, q), *range(2 * q, n)]
    else:
        seq, groups, sends = list(range(n)), [(0, n)], list(range(n - 1, 0, -1))
    count = groups[0][1]
    spread = max(rem, 1) * half // 128
    anywhere = pl.BlockSpec(memory_space=pl.ANY)
    main = pltpu.VMEM((n, base, half), bf16)
    extra = pltpu.VMEM((n, spread, 128), bf16)
    exchange = pltpu.VMEM((len(groups), count * (base + rem), half), bf16)
    dma = pltpu.SemaphoreType.DMA
    sems = dma((2 * n,))
    return pl.pallas_call(
        functools.partial(kernel, n, base, rem, seq, groups, sends),
        out_shape=jax.ShapeDtypeStruct((toks, half), bf16),
        in_specs=[anywhere] * 8,
        out_specs=pl.BlockSpec(memory_space=pltpu.VMEM),
        scratch_shapes=[
            pltpu.VMEM((toks, half), bf16),
            pltpu.VMEM((top, toks), jnp.int32),
            pltpu.VMEM((top, toks), f32),
            pltpu.VMEM((2, 2, 1, half), f32),
            pltpu.VMEM((2, half, ff), bf16),
            pltpu.VMEM((2, half, ff), bf16),
            pltpu.VMEM((2, ff, half), bf16),
            main, extra,
            pltpu.VMEM((2, n, base, half), bf16),
            pltpu.VMEM((2, n, spread, 128), bf16),
            exchange, exchange,
            main, extra, main, extra,
            dma((5,)), dma((6,)), dma((2,)),
            sems, sems, sems, sems, dma((len(groups),)), dma((len(groups),)), sems, sems,
        ],
        compiler_params=pltpu.CompilerParams(collective_id=0, has_side_effects=True),
    )(
        tokens, routes.T, gate_logits.T, norm_gain.reshape(1, half), norm_shift.reshape(1, half),
        gate_weight, up_weight, down_weight,
    )


def solution(mesh):
    placed = (
        P(("grp", "ep"), "tp"),
        P(("grp", "ep"), None),
        P(("grp", "ep"), None),
        P("tp"),
        P("tp"),
        P("ep", None, "tp"),
        P("ep", None, "tp"),
        P("ep", "tp", None),
    )
    return jax.shard_map(
        body, mesh=mesh, in_specs=placed, out_specs=P(("grp", "ep"), "tp"), check_vma=False
    )
```

```python
import functools

import jax
import jax.numpy as jnp
from jax import lax
from jax.experimental import pallas as pl
from jax.experimental.pallas import tpu as pltpu
from jax.sharding import PartitionSpec as P

norm_eps = 1e-05
clamp_limit = 7.0
sigmoid_slope = 1.702
MESH = pl.DeviceIdType.MESH
LANES = 128
f32 = jnp.float32
bf16 = jnp.bfloat16


def dot(a, b):
    return jnp.dot(a, b, preferred_element_type=f32)


def iota(shape, axis):
    return lax.broadcasted_iota(jnp.int32, shape, axis)


def kernel(
    n, base, rem, seq, groups, sends,
    tokens_hbm, routes_hbm, logits_hbm, gain_hbm, shift_hbm, wg_hbm, wu_hbm, wd_hbm,
    out_ref,
    tok, routes_ref, logits_ref, affine, wg, wu, wd,
    outb1, outb2, rows1, rows2, part_out, part_in, ans1, ans2, back1, back2,
    i_sem, w_sem, a_sem, d_send, d_recv, f_send, f_recv, p_send, p_recv, r_send, r_recv, ready,
):
    me = lax.axis_index("ep")
    tp = lax.axis_index("tp")
    other = 1 - tp
    toks, half = tok.shape
    width = 2 * half
    top = routes_ref.shape[0]
    chunks = half // LANES
    spread = rem * chunks
    paired = n & (n - 1) == 0
    parts = 2 if rem else 1

    def peer(d, sign):
        if not paired:
            return lax.rem(me + sign * d + n, n)
        where, bit = me, 1
        while bit < n:
            if d & bit:
                where = where + bit * (1 - 2 * lax.rem(me // bit, 2))
            bit *= 2
        return where

    target = [peer(d, 1) for d in seq]
    source = [peer(d, -1) for d in seq]

    barrier = pltpu.get_barrier_semaphore()
    staged = paired and n >= 4
    greeted = [i for i in sends if seq[i] <= n // 2] if staged else sends
    for i in greeted:
        pl.semaphore_signal(barrier, inc=1, device_id={"ep": target[i]}, device_id_type=MESH)
    pl.semaphore_signal(barrier, inc=1, device_id={"tp": other}, device_id_type=MESH)

    first = [
        pltpu.make_async_copy(routes_hbm, routes_ref, i_sem.at[0]),
        pltpu.make_async_copy(tokens_hbm, tok, i_sem.at[1]),
        pltpu.make_async_copy(logits_hbm, logits_ref, i_sem.at[2]),
        pltpu.make_async_copy(gain_hbm, affine.at[0, 0], i_sem.at[3]),
        pltpu.make_async_copy(shift_hbm, affine.at[0, 1], i_sem.at[4]),
    ]
    loads = []
    for j, side in enumerate((tp, other)):
        span = pl.ds(pl.multiple_of(side * half, half), half)
        loads += [
            pltpu.make_async_copy(wg_hbm.at[0, span], wg.at[j], w_sem.at[3 * j]),
            pltpu.make_async_copy(wu_hbm.at[0, span], wu.at[j], w_sem.at[3 * j + 1]),
            pltpu.make_async_copy(wd_hbm.at[0, :, span], wd.at[j], w_sem.at[3 * j + 2]),
        ]
    for load in first + loads:
        load.start()
    for load in first:
        load.wait()

    routes = routes_ref[...]
    logits = jnp.exp(logits_ref[...])
    weights = logits / jnp.sum(logits, axis=0, keepdims=True)
    before = jnp.where(iota((toks, toks), 0) < iota((toks, toks), 1), 1.0, 0.0).astype(bf16)

    def choose(place, rank):
        shape = place.shape
        expert = jnp.zeros(shape, jnp.int32)
        for i in range(n):
            expert = jnp.where(place == i, target[i], expert)
        named = jnp.zeros(shape, f32)
        share = jnp.zeros(shape, f32)
        for k in range(top):
            hit = routes[k:k + 1, :] == expert
            named = jnp.where(hit, 1.0, named)
            share = jnp.where(hit, weights[k:k + 1, :], share)
        chosen = (named > 0.5) & (dot(named.astype(bf16), before) == rank.astype(f32))
        return jnp.where(chosen, 1.0, 0.0), jnp.where(chosen, share, 0.0)

    def split(share):
        whole = jnp.transpose(share)
        a = whole.astype(bf16)
        rest = whole - a.astype(f32)
        b = rest.astype(bf16)
        return a, b, (rest - b.astype(f32)).astype(bf16)

    row = iota((n * base, toks), 0)
    pick, share = choose(row // base, row % base)
    outb1[...] = dot(pick.astype(bf16), tok[...]).astype(bf16).reshape(n, base, half)
    share_main = split(share)
    if rem:
        row = iota((n * spread, toks), 0)
        pick, _ = choose(row // spread, base + row % rem)
        chunk = row % spread // rem
        total = jnp.zeros((n * spread, LANES), f32)
        for c in range(chunks):
            total += dot(
                jnp.where(chunk == c, pick, 0.0).astype(bf16), tok[:, c * LANES:(c + 1) * LANES]
            )
        outb2[...] = total.astype(bf16).reshape(n, spread, LANES)
        row = iota((n * rem, toks), 0)
        _, share = choose(row // rem, base + row % rem)
        share_extra = split(share)

    def unpack(flat, count):
        size = count * spread
        r, z = iota((size, size), 0), iota((size, size), 1)
        c, q = r // (count * rem), r % (count * rem)
        where = q // rem * spread + c * rem + q % rem
        rows = dot(jnp.where(where == z, 1.0, 0.0).astype(bf16), flat)
        block = count * rem
        return jnp.concatenate([rows[c * block:(c + 1) * block] for c in range(chunks)], axis=1)

    def repack(rows, count):
        size = count * spread
        z, r = iota((size, size), 0), iota((size, size), 1)
        c, q = r // (count * rem), r % (count * rem)
        where = q // rem * spread + c * rem + q % rem
        flat = jnp.concatenate(
            [rows[:, c * LANES:(c + 1) * LANES] for c in range(chunks)], axis=0
        ).astype(bf16)
        return dot(jnp.where(where == z, 1.0, 0.0).astype(bf16), flat).astype(bf16)

    def across(src, dst, i, part, send, recv, place):
        return pltpu.make_async_remote_copy(
            src, dst, send.at[2 * i + part], recv.at[2 * i + part], device_id=place,
            device_id_type=MESH,
        )

    def dispatch(i):
        place = {"ep": target[i]}
        pieces = [(outb1, rows1), (outb2, rows2)][:parts]
        return [
            across(a.at[i], b.at[0, i], i, p, d_send, d_recv, place)
            for p, (a, b) in enumerate(pieces)
        ]

    def forward(i):
        place = {"tp": other}
        pieces = [(outb1, rows1), (outb2, rows2)][:parts]
        return [
            across(b.at[0, i] if i else a.at[i], b.at[1, i], i, p, f_send, f_recv, place)
            for p, (a, b) in enumerate(pieces)
        ]

    def give_back(i):
        place = {"ep": source[i]}
        pieces = [(ans1, back1), (ans2, back2)][:parts]
        return [
            across(a.at[i], b.at[i], i, p, r_send, r_recv, place)
            for p, (a, b) in enumerate(pieces)
        ]

    def partial(g):
        return pltpu.make_async_remote_copy(
            part_out.at[g], part_in.at[g], p_send.at[g], p_recv.at[g], device_id={"tp": other},
            device_id_type=MESH,
        )

    affine_copy = pltpu.make_async_remote_copy(
        affine.at[0], affine.at[1], a_sem.at[0], a_sem.at[1], device_id={"tp": other},
        device_id_type=MESH,
    )

    pl.semaphore_wait(barrier, len(greeted) + 1)
    if staged:
        for i in greeted:
            if seq[i] < n // 2:
                pl.semaphore_signal(
                    ready.at[seq[i]], inc=1, device_id={"ep": target[i]}, device_id_type=MESH
                )
    started = 0
    for i in sends:
        if staged and seq[i] > n // 2:
            pl.semaphore_wait(ready.at[seq[i] - n // 2], 1)
        for copy in dispatch(i):
            copy.start()
        if not started:
            for copy in forward(0):
                copy.start()
            affine_copy.start()
            started = 1
    rows1[0, 0] = outb1[0]
    if rem:
        rows2[0, 0] = outb2[0]
    for load in loads:
        load.wait()
    affine_copy.wait_recv()

    def landed(g):
        lower, upper = groups[g]
        for i in [i for i in [0] + sends if lower <= i < upper and i]:
            for arrived, onward in zip(dispatch(i), forward(i)):
                arrived.wait_recv()
                onward.start()

    def gathered(j, lower, upper):
        count = upper - lower
        main = rows1[j, lower:upper].reshape(count * base, half).astype(f32)
        if not rem:
            return main
        extra = unpack(rows2[j, lower:upper].reshape(count * spread, LANES), count)
        return jnp.concatenate([main, extra], axis=0)

    def experts(g):
        lower, upper = groups[g]
        for i in range(lower, upper):
            for copy in forward(i):
                copy.wait_recv()
        x = [gathered(j, lower, upper) for j in range(2)]
        average = (
            jnp.sum(x[0], axis=1, keepdims=True) + jnp.sum(x[1], axis=1, keepdims=True)
        ) / width
        squares = (
            jnp.sum(x[0] * x[0], axis=1, keepdims=True)
            + jnp.sum(x[1] * x[1], axis=1, keepdims=True)
        ) / width
        scale = lax.rsqrt(squares - average * average + norm_eps)
        normed = [
            ((x[j] - average) * scale * affine[j, 0] + affine[j, 1]).astype(bf16)
            for j in range(2)
        ]
        gate = dot(normed[0], wg[0]) + dot(normed[1], wg[1])
        up = dot(normed[0], wu[0]) + dot(normed[1], wu[1])
        cut = jnp.minimum(gate, clamp_limit)
        hidden = (
            (jnp.clip(up, -clamp_limit, clamp_limit) + 1.0)
            * cut * jax.nn.sigmoid(sigmoid_slope * cut)
        ).astype(bf16)
        part_out[g] = dot(hidden, wd[1]).astype(bf16)
        partial(g).start()
        return dot(hidden, wd[0]).astype(bf16)

    def answer(g, mine):
        lower, upper = groups[g]
        count = upper - lower
        partial(g).wait_recv()
        total = (mine.astype(f32) + part_in[g].astype(f32)).astype(bf16)
        ans1[lower:upper] = total[:count * base].reshape(count, base, half)
        if rem:
            ans2[lower:upper] = repack(total[count * base:].astype(f32), count).reshape(
                count, spread, LANES
            )
        if lower == 0:
            back1[0] = ans1[0]
            if rem:
                back2[0] = ans2[0]
        for i in sends:
            if lower <= i < upper:
                for copy in give_back(i):
                    copy.start()

    landed(0)
    for g in range(len(groups)):
        mine = experts(g)
        if g + 1 < len(groups):
            landed(g + 1)
        answer(g, mine)
    for i in sends:
        for copy in give_back(i):
            copy.wait_recv()
    got = back1[...].reshape(n * base, half)
    mixed = dot(share_main[2], got) + dot(share_main[1], got) + dot(share_main[0], got)
    if rem:
        got = unpack(back2[...].reshape(n * spread, LANES), n).astype(bf16)
        mixed += dot(share_extra[2], got) + dot(share_extra[1], got) + dot(share_extra[0], got)
    out_ref[...] = mixed.astype(bf16)
    affine_copy.wait_send()
    for g in range(len(groups)):
        partial(g).wait_send()
    for i in range(n):
        for copy in forward(i) + (dispatch(i) + give_back(i) if i else []):
            copy.wait_send()


def body(tokens, routes, gate_logits, norm_gain, norm_shift, gate_weight, up_weight, down_weight):
    n = lax.axis_size("ep")
    toks, top = routes.shape
    half = tokens.shape[1]
    cap = toks * top // n + 2
    base, rem = cap // 8 * 8, cap % 8
    if base == 0 or rem > 4:
        base, rem = -(-cap // 8) * 8, 0
    ff = gate_weight.shape[2]
    if n % 4 == 0:
        q = n // 4
        seq = [*range(q), *range(2 * q, 3 * q), *range(3 * q, n), *range(q, 2 * q)]
        groups = [(0, 2 * q), (2 * q, n)]
        sends = [q, *range(1, q), *range(q + 1, 2 * q), *range(2 * q, n)]
    else:
        seq, groups, sends = list(range(n)), [(0, n)], list(range(n - 1, 0, -1))
    count = groups[0][1]
    spread = max(rem, 1) * half // 128
    anywhere = pl.BlockSpec(memory_space=pl.ANY)
    main = pltpu.VMEM((n, base, half), bf16)
    extra = pltpu.VMEM((n, spread, 128), bf16)
    exchange = pltpu.VMEM((len(groups), count * (base + rem), half), bf16)
    dma = pltpu.SemaphoreType.DMA
    sems = dma((2 * n,))
    return pl.pallas_call(
        functools.partial(kernel, n, base, rem, seq, groups, sends),
        out_shape=pltpu.VMEM((toks, half), bf16),
        in_specs=[anywhere] * 8,
        out_specs=pl.BlockSpec(memory_space=pltpu.VMEM),
        scratch_shapes=[
            pltpu.VMEM((toks, half), bf16),
            pltpu.VMEM((top, toks), jnp.int32),
            pltpu.VMEM((top, toks), f32),
            pltpu.VMEM((2, 2, 1, half), f32),
            pltpu.VMEM((2, half, ff), bf16),
            pltpu.VMEM((2, half, ff), bf16),
            pltpu.VMEM((2, ff, half), bf16),
            main, extra,
            pltpu.VMEM((2, n, base, half), bf16),
            pltpu.VMEM((2, n, spread, 128), bf16),
            exchange, exchange,
            main, extra, main, extra,
            dma((5,)), dma((6,)), dma((2,)),
            sems, sems, sems, sems, dma((len(groups),)), dma((len(groups),)), sems, sems,
            pltpu.SemaphoreType.REGULAR((n,)),
        ],
        compiler_params=pltpu.CompilerParams(collective_id=0, has_side_effects=True),
    )(
        tokens, routes.T, gate_logits.T, norm_gain.reshape(1, half), norm_shift.reshape(1, half),
        gate_weight, up_weight, down_weight,
    )


def solution(mesh):
    placed = (
        P(("grp", "ep"), "tp"),
        P(("grp", "ep"), None),
        P(("grp", "ep"), None),
        P("tp"),
        P("tp"),
        P("ep", None, "tp"),
        P("ep", None, "tp"),
        P("ep", "tp", None),
    )
    return jax.shard_map(
        body, mesh=mesh, in_specs=placed, out_specs=P(("grp", "ep"), "tp"), check_vma=False
    )
```

```python
import functools

import jax
import jax.numpy as jnp
from jax import lax
from jax.experimental import pallas as pl
from jax.experimental.pallas import tpu as pltpu
from jax.sharding import PartitionSpec as P

norm_eps = 1e-05
clamp_limit = 7.0
sigmoid_slope = 1.702
MESH = pl.DeviceIdType.MESH
LANES = 128
f32 = jnp.float32
bf16 = jnp.bfloat16


def dot(a, b):
    return jnp.dot(a, b, preferred_element_type=f32)


def iota(shape, axis):
    return lax.broadcasted_iota(jnp.int32, shape, axis)


def kernel(
    n, base, rem, seq, groups, sends,
    tokens_hbm, routes_hbm, logits_hbm, gain_hbm, shift_hbm, wg_hbm, wu_hbm, wd_hbm,
    out_ref,
    tok, routes_ref, logits_ref, affine, wg, wu, wd,
    outb1, outb2, rows1, rows2, part_out, part_in, ans1, ans2, back1, back2,
    i_sem, w_sem, a_sem, d_send, d_recv, f_send, f_recv, p_send, p_recv, r_send, r_recv, ready,
):
    me = lax.axis_index("ep")
    tp = lax.axis_index("tp")
    other = 1 - tp
    toks, half = tok.shape
    width = 2 * half
    top = routes_ref.shape[0]
    chunks = half // LANES
    spread = rem * chunks
    paired = n & (n - 1) == 0
    parts = 2 if rem else 1

    def peer(d, sign):
        if not paired:
            return lax.rem(me + sign * d + n, n)
        where, bit = me, 1
        while bit < n:
            if d & bit:
                where = where + bit * (1 - 2 * lax.rem(me // bit, 2))
            bit *= 2
        return where

    sizes = [((b - a) * (base + rem), -(-(b - a) * (base + rem) // 8) * 8) for a, b in groups]
    target = [peer(d, 1) for d in seq]
    source = [peer(d, -1) for d in seq]

    barrier = pltpu.get_barrier_semaphore()
    staged = paired and n >= 4
    greeted = [i for i in sends if seq[i] <= n // 2] if staged else sends
    for i in greeted:
        pl.semaphore_signal(barrier, inc=1, device_id={"ep": target[i]}, device_id_type=MESH)
    pl.semaphore_signal(barrier, inc=1, device_id={"tp": other}, device_id_type=MESH)

    first = [
        pltpu.make_async_copy(routes_hbm, routes_ref, i_sem.at[0]),
        pltpu.make_async_copy(tokens_hbm, tok, i_sem.at[1]),
        pltpu.make_async_copy(logits_hbm, logits_ref, i_sem.at[2]),
        pltpu.make_async_copy(gain_hbm, affine.at[0, 0], i_sem.at[3]),
        pltpu.make_async_copy(shift_hbm, affine.at[0, 1], i_sem.at[4]),
    ]
    loads = []
    for j, side in enumerate((tp, other)):
        span = pl.ds(pl.multiple_of(side * half, half), half)
        loads += [
            pltpu.make_async_copy(wg_hbm.at[0, span], wg.at[j], w_sem.at[3 * j]),
            pltpu.make_async_copy(wu_hbm.at[0, span], wu.at[j], w_sem.at[3 * j + 1]),
            pltpu.make_async_copy(wd_hbm.at[0, :, span], wd.at[j], w_sem.at[3 * j + 2]),
        ]
    for load in first + loads:
        load.start()
    for load in first:
        load.wait()

    routes = routes_ref[...]
    logits = jnp.exp(logits_ref[...])
    weights = logits / jnp.sum(logits, axis=0, keepdims=True)
    before = jnp.where(iota((toks, toks), 0) < iota((toks, toks), 1), 1.0, 0.0).astype(bf16)

    def choose(place, rank):
        shape = place.shape
        expert = jnp.zeros(shape, jnp.int32)
        for i in range(n):
            expert = jnp.where(place == i, target[i], expert)
        named = jnp.zeros(shape, f32)
        share = jnp.zeros(shape, f32)
        for k in range(top):
            hit = routes[k:k + 1, :] == expert
            named = jnp.where(hit, 1.0, named)
            share = jnp.where(hit, weights[k:k + 1, :], share)
        chosen = (named > 0.5) & (dot(named.astype(bf16), before) == rank.astype(f32))
        return jnp.where(chosen, 1.0, 0.0), jnp.where(chosen, share, 0.0)

    def split(share):
        whole = jnp.transpose(share)
        a = whole.astype(bf16)
        rest = whole - a.astype(f32)
        b = rest.astype(bf16)
        return a, b, (rest - b.astype(f32)).astype(bf16)

    row = iota((n * base, toks), 0)
    pick, share = choose(row // base, row % base)
    outb1[...] = dot(pick.astype(bf16), tok[...]).astype(bf16).reshape(n, base, half)
    share_main = [split(share[lower * base:upper * base]) for lower, upper in groups]
    if rem:
        row = iota((n * spread, toks), 0)
        pick, _ = choose(row // spread, base + row % rem)
        chunk = row % spread // rem
        total = jnp.zeros((n * spread, LANES), f32)
        for c in range(chunks):
            total += dot(
                jnp.where(chunk == c, pick, 0.0).astype(bf16), tok[:, c * LANES:(c + 1) * LANES]
            )
        outb2[...] = total.astype(bf16).reshape(n, spread, LANES)
        row = iota((n * rem, toks), 0)
        _, share = choose(row // rem, base + row % rem)
        share_extra = [split(share[lower * rem:upper * rem]) for lower, upper in groups]

    def unpack(flat, count):
        size = count * spread
        r, z = iota((size, size), 0), iota((size, size), 1)
        c, q = r // (count * rem), r % (count * rem)
        where = q // rem * spread + c * rem + q % rem
        rows = dot(jnp.where(where == z, 1.0, 0.0).astype(bf16), flat)
        block = count * rem
        return jnp.concatenate([rows[c * block:(c + 1) * block] for c in range(chunks)], axis=1)

    def repack(rows, count):
        size = count * spread
        z, r = iota((size, size), 0), iota((size, size), 1)
        c, q = r // (count * rem), r % (count * rem)
        where = q // rem * spread + c * rem + q % rem
        flat = jnp.concatenate(
            [rows[:, c * LANES:(c + 1) * LANES] for c in range(chunks)], axis=0
        ).astype(bf16)
        return dot(jnp.where(where == z, 1.0, 0.0).astype(bf16), flat).astype(bf16)

    def across(src, dst, i, part, send, recv, place):
        return pltpu.make_async_remote_copy(
            src, dst, send.at[2 * i + part], recv.at[2 * i + part], device_id=place,
            device_id_type=MESH,
        )

    def dispatch(i):
        place = {"ep": target[i]}
        pieces = [(outb1, rows1), (outb2, rows2)][:parts]
        return [
            across(a.at[i], b.at[0, i], i, p, d_send, d_recv, place)
            for p, (a, b) in enumerate(pieces)
        ]

    def forward(i):
        place = {"tp": other}
        pieces = [(outb1, rows1), (outb2, rows2)][:parts]
        return [
            across(b.at[0, i] if i else a.at[i], b.at[1, i], i, p, f_send, f_recv, place)
            for p, (a, b) in enumerate(pieces)
        ]

    def give_back(i):
        place = {"ep": source[i]}
        pieces = [(ans1, back1), (ans2, back2)][:parts]
        return [
            across(a.at[i], b.at[i], i, p, r_send, r_recv, place)
            for p, (a, b) in enumerate(pieces)
        ]

    def partial(g):
        return pltpu.make_async_remote_copy(
            part_out.at[g, pl.ds(0, sizes[g][1])], part_in.at[g, pl.ds(0, sizes[g][1])], p_send.at[g], p_recv.at[g], device_id={"tp": other},
            device_id_type=MESH,
        )

    affine_copy = pltpu.make_async_remote_copy(
        affine.at[0], affine.at[1], a_sem.at[0], a_sem.at[1], device_id={"tp": other},
        device_id_type=MESH,
    )

    pl.semaphore_wait(barrier, len(greeted) + 1)
    if staged:
        for i in greeted:
            if seq[i] < n // 2:
                pl.semaphore_signal(
                    ready.at[seq[i]], inc=1, device_id={"ep": target[i]}, device_id_type=MESH
                )
    started = 0
    for i in sends:
        if staged and seq[i] > n // 2:
            pl.semaphore_wait(ready.at[seq[i] - n // 2], 1)
        for copy in dispatch(i):
            copy.start()
        if not started:
            for copy in forward(0):
                copy.start()
            affine_copy.start()
            started = 1
    rows1[0, 0] = outb1[0]
    if rem:
        rows2[0, 0] = outb2[0]
    for load in loads:
        load.wait()
    affine_copy.wait_recv()

    def landed(g):
        lower, upper = groups[g]
        for i in [i for i in [0] + sends if lower <= i < upper and i]:
            for arrived, onward in zip(dispatch(i), forward(i)):
                arrived.wait_recv()
                onward.start()

    def gathered(j, lower, upper):
        count = upper - lower
        main = rows1[j, lower:upper].reshape(count * base, half).astype(f32)
        if not rem:
            return main
        extra = unpack(rows2[j, lower:upper].reshape(count * spread, LANES), count)
        return jnp.concatenate([main, extra], axis=0)

    def experts(g):
        lower, upper = groups[g]
        for i in range(lower, upper):
            for copy in forward(i):
                copy.wait_recv()
        x = [gathered(j, lower, upper) for j in range(2)]
        average = (
            jnp.sum(x[0], axis=1, keepdims=True) + jnp.sum(x[1], axis=1, keepdims=True)
        ) / width
        squares = (
            jnp.sum(x[0] * x[0], axis=1, keepdims=True)
            + jnp.sum(x[1] * x[1], axis=1, keepdims=True)
        ) / width
        scale = lax.rsqrt(squares - average * average + norm_eps)
        normed = [
            ((x[j] - average) * scale * affine[j, 0] + affine[j, 1]).astype(bf16)
            for j in range(2)
        ]
        gate = dot(normed[0], wg[0]) + dot(normed[1], wg[1])
        up = dot(normed[0], wu[0]) + dot(normed[1], wu[1])
        cut = jnp.minimum(gate, clamp_limit)
        hidden = (
            (jnp.clip(up, -clamp_limit, clamp_limit) + 1.0)
            * cut * jax.nn.sigmoid(sigmoid_slope * cut)
        ).astype(bf16)
        part_out[g, :sizes[g][0]] = dot(hidden, wd[1]).astype(bf16)
        partial(g).start()
        return dot(hidden, wd[0]).astype(bf16)

    def answer(g, mine):
        lower, upper = groups[g]
        count = upper - lower
        partial(g).wait_recv()
        total = (mine.astype(f32) + part_in[g, :sizes[g][0]].astype(f32)).astype(bf16)
        ans1[lower:upper] = total[:count * base].reshape(count, base, half)
        for i in sends:
            if lower <= i < upper:
                give_back(i)[0].start()
        if rem:
            ans2[lower:upper] = repack(total[count * base:].astype(f32), count).reshape(
                count, spread, LANES
            )
        if lower == 0:
            back1[0] = ans1[0]
            if rem:
                back2[0] = ans2[0]
        for i in sends:
            if lower <= i < upper:
                for copy in give_back(i)[1:]:
                    copy.start()

    landed(0)
    for g in range(len(groups)):
        mine = experts(g)
        if g + 1 < len(groups):
            landed(g + 1)
        answer(g, mine)
    mixed = jnp.zeros((toks, half), f32)
    for g, (lower, upper) in enumerate(groups):
        for i in sends:
            if lower <= i < upper:
                for copy in give_back(i):
                    copy.wait_recv()
        count = upper - lower
        got = back1[lower:upper].reshape(count * base, half)
        for piece in reversed(share_main[g]):
            mixed += dot(piece, got)
        if rem:
            got = unpack(back2[lower:upper].reshape(count * spread, LANES), count).astype(bf16)
            for piece in reversed(share_extra[g]):
                mixed += dot(piece, got)
    out_ref[...] = mixed.astype(bf16)
    affine_copy.wait_send()
    for g in range(len(groups)):
        partial(g).wait_send()
    for i in range(n):
        for copy in forward(i) + (dispatch(i) + give_back(i) if i else []):
            copy.wait_send()


def body(tokens, routes, gate_logits, norm_gain, norm_shift, gate_weight, up_weight, down_weight):
    n = lax.axis_size("ep")
    toks, top = routes.shape
    half = tokens.shape[1]
    cap = toks * top // n + 2
    base, rem = cap // 8 * 8, cap % 8
    if base == 0 or rem > 4:
        base, rem = -(-cap // 8) * 8, 0
    ff = gate_weight.shape[2]
    if n % 4 == 0:
        q = n // 4
        seq = [*range(q), *range(2 * q, 3 * q), *range(q, 2 * q), *range(3 * q, n)]
        groups = [(0, 3 * q), (3 * q, n)]
        sends = [q, *range(1, q), *range(q + 1, 2 * q), *range(2 * q, n)]
    else:
        seq, groups, sends = list(range(n)), [(0, n)], list(range(n - 1, 0, -1))
    count = groups[0][1]
    spread = max(rem, 1) * half // 128
    anywhere = pl.BlockSpec(memory_space=pl.ANY)
    main = pltpu.VMEM((n, base, half), bf16)
    extra = pltpu.VMEM((n, spread, 128), bf16)
    exchange = pltpu.VMEM((len(groups), -(-count * (base + rem) // 8) * 8, half), bf16)
    dma = pltpu.SemaphoreType.DMA
    sems = dma((2 * n,))
    return pl.pallas_call(
        functools.partial(kernel, n, base, rem, seq, groups, sends),
        out_shape=pltpu.VMEM((toks, half), bf16),
        in_specs=[anywhere] * 8,
        out_specs=pl.BlockSpec(memory_space=pltpu.VMEM),
        scratch_shapes=[
            pltpu.VMEM((toks, half), bf16),
            pltpu.VMEM((top, toks), jnp.int32),
            pltpu.VMEM((top, toks), f32),
            pltpu.VMEM((2, 2, 1, half), f32),
            pltpu.VMEM((2, half, ff), bf16),
            pltpu.VMEM((2, half, ff), bf16),
            pltpu.VMEM((2, ff, half), bf16),
            main, extra,
            pltpu.VMEM((2, n, base, half), bf16),
            pltpu.VMEM((2, n, spread, 128), bf16),
            exchange, exchange,
            main, extra, main, extra,
            dma((5,)), dma((6,)), dma((2,)),
            sems, sems, sems, sems, dma((len(groups),)), dma((len(groups),)), sems, sems,
            pltpu.SemaphoreType.REGULAR((n,)),
        ],
        compiler_params=pltpu.CompilerParams(collective_id=0, has_side_effects=True),
    )(
        tokens, routes.T, gate_logits.T, norm_gain.reshape(1, half), norm_shift.reshape(1, half),
        gate_weight, up_weight, down_weight,
    )


def solution(mesh):
    placed = (
        P(("grp", "ep"), "tp"),
        P(("grp", "ep"), None),
        P(("grp", "ep"), None),
        P("tp"),
        P("tp"),
        P("ep", None, "tp"),
        P("ep", None, "tp"),
        P("ep", "tp", None),
    )
    return jax.shard_map(
        body, mesh=mesh, in_specs=placed, out_specs=P(("grp", "ep"), "tp"), check_vma=False
    )
```
